32 devices in a mesh: fs: 16 (over z, y, x), tp: 2 (over core).
Axes of the slice: x: 2, y: 2, z: 4, core: 2. Of those that a mesh axis runs over, the one named last changes fastest.
Arguments:
- tokens: bfloat16 [6144, 2048], P('fs', 'tp'), may hold values from -24 to 24, as said below
- mixer_gain: float32 [2048], replicated, may hold values from 0.1 to 1.9
- w_content: float32 [2048, 1024], P('fs', 'tp'), may hold values from -0.125 to 0.125
- w_spatial: float32 [2048, 1024], P('fs', 'tp'), may hold values from -0.125 to 0.125
- content_scale: float32 [1024], P('tp'), may hold values from 0.5 to 2
- spatial_scale: float32 [1024], P('tp'), may hold values from 0.2 to 3.5, as said below
- spatial_gain: float32 [1024], P('tp'), may hold values from 0.1 to 1.9
- block_mixing: bfloat16 [8, 128, 128], P('tp'), may hold values from -0.5 to 0.5
- block_bias: float32 [8, 128], P('tp'), may hold values from -6 to 6
- w_project: float32 [1024, 2048], P('tp', 'fs'), may hold values from -0.1875 to 0.1875
- project_scale: float32 [2048], P('fs'), may hold values from 0.5 to 2
- channel_gain: float32 [2048], replicated, may hold values from 0.1 to 1.9
- w_up: float32 [2048, 8192], P('fs', 'tp'), may hold values from -0.125 to 0.125
- up_scale: float32 [8192], P('tp'), may hold values from 0.5 to 2
- w_down: float32 [8192, 2048], P('tp', 'fs'), may hold values from -0.0625 to 0.0625
- down_scale: float32 [2048], P('fs'), may hold values from 0.5 to 2
Outputs:
- layer_out: bfloat16 [6144, 2048], P('fs', 'tp')
The draws below stay inside these ranges and needn't reach their ends.
Inputs may be any that keep to these rules, and one draw needn't show every extreme that they name: `tokens`: activations whose features and rows have differing scales. `spatial_scale`: positive column scales.
All inputs are finite; a program needn't handle non-finite values.
Results may differ from the reference program's by a relative error of at most 0.019.
Values may be sent and summed in bfloat16 or wider, within the bound.
No kernel may reach another device: no remote copies, remote signals or barrier semaphores. Data moves between devices by JAX's collectives and lax.ppermute only.
A program may use at most 128 MiB of HBM per device.

```python
import math
import jax
import jax.numpy as jnp
from jax import lax

D = 2048
GROUPS = 8
GCH = 128
W_SGU = 1024
FF = 8192
BLOCK = 128
TOK_DEV = 384
TOKENS = 6144
N_FS = 16
N_TP = 2


def draw_tokens(key, part):
    first_key = jax.random.fold_in(key, 11)
    second_key = jax.random.fold_in(key, 12)
    third_key = jax.random.fold_in(key, 13)
    column_scales = jnp.exp(jax.random.uniform(second_key, (D,), jnp.float32, math.log(0.3), math.log(3.0)))
    base_values = jax.random.truncated_normal(first_key, -4.0, 4.0, (TOKENS, D), jnp.float32)
    row_scales = jnp.exp(jax.random.uniform(third_key, (TOKENS, 1), jnp.float32, math.log(0.5), math.log(2.0)))
    return (base_values * column_scales[None, :] * row_scales).astype(jnp.bfloat16)


def draw_spatial_scale(key, part):
    jitter_key = jax.random.fold_in(key, 21)
    position = jnp.arange(W_SGU).astype(jnp.float32) / (W_SGU - 1)
    jitter = jnp.exp(jax.random.uniform(jitter_key, (W_SGU,), jnp.float32, -0.35, 0.35))
    base_scale = jnp.exp(math.log(0.5) + (math.log(1.6) - math.log(0.5)) * position)
    return (base_scale * jitter).astype(jnp.float32)


def shard_levels(own_key, dims, shards, smallest, largest):
    factor_of = 1.0
    for dim, blocks in shards:
        heights = jax.random.uniform(jax.random.fold_in(jax.random.fold_in(own_key, 6), dim), (blocks,), jnp.float32, smallest / len(shards), largest / len(shards))
        factor_of = factor_of * jnp.repeat(jnp.exp(heights), dims[dim] // blocks).reshape((-1,) + (1,) * (len(dims) - 1 - dim))
    return factor_of


def scatter_about(stream_key, dims, scale, reach, split=(), kind=jnp.bfloat16):
    values = scale * jax.random.normal(stream_key, dims, jnp.float32)
    if split:
        values = values * shard_levels(stream_key, dims, split, -0.22, 0.18)
    return jnp.clip(values, -reach, reach).astype(kind)


def setup_inputs(seed: int = 0) -> dict:
    seeds = jax.random.split(jax.random.key(seed), 17)
    return {
        "tokens": draw_tokens(jax.random.fold_in(seeds[16], 71), 0),
        "mixer_gain": jnp.clip(1.0 + 0.18 * jax.random.normal(seeds[1], (D,), jnp.float32), 0.1, 1.9),
        "w_content": scatter_about(seeds[2], (D, W_SGU), D ** -0.5, 0.125, ((0, 16), (1, 2)), jnp.float32),
        "w_spatial": scatter_about(seeds[3], (D, W_SGU), D ** -0.5, 0.125, ((0, 16), (1, 2)), jnp.float32),
        "content_scale": jnp.clip(jnp.exp(math.log(2.0) - 1.3862944 * jax.random.uniform(seeds[4], (W_SGU,), jnp.float32) ** shard_levels(seeds[4], (W_SGU,), ((0, 2),), -0.2, 0.2)), 0.5, 2.0),
        "spatial_scale": draw_spatial_scale(jax.random.fold_in(seeds[16], 71), 0),
        "spatial_gain": jnp.clip(1.0 + 0.18 * jax.random.normal(seeds[6], (W_SGU,), jnp.float32), 0.1, 1.9),
        "block_mixing": scatter_about(seeds[7], (GROUPS, BLOCK, BLOCK), BLOCK ** -0.5, 0.5, ((0, 2),)),
        "block_bias": scatter_about(seeds[8], (GROUPS, BLOCK), 1.0, 6.0, ((0, 2),), jnp.float32),
        "w_project": scatter_about(seeds[9], (W_SGU, D), W_SGU ** -0.5, 0.1875, ((0, 2), (1, 16)), jnp.float32),
        "project_scale": jnp.clip(jnp.exp(math.log(2.0) - 1.3862944 * jax.random.uniform(seeds[10], (D,), jnp.float32) ** shard_levels(seeds[10], (D,), ((0, 16),), -0.2, 0.2)), 0.5, 2.0),
        "channel_gain": jnp.clip(1.0 + 0.18 * jax.random.normal(seeds[11], (D,), jnp.float32), 0.1, 1.9),
        "w_up": scatter_about(seeds[12], (D, FF), D ** -0.5, 0.125, ((0, 16), (1, 2)), jnp.float32),
        "up_scale": jnp.clip(jnp.exp(math.log(2.0) - 1.3862944 * jax.random.uniform(seeds[13], (FF,), jnp.float32) ** shard_levels(seeds[13], (FF,), ((0, 2),), -0.2, 0.2)), 0.5, 2.0),
        "w_down": scatter_about(seeds[14], (FF, D), FF ** -0.5, 0.0625, ((0, 2), (1, 16)), jnp.float32),
        "down_scale": jnp.clip(jnp.exp(math.log(2.0) - 1.3862944 * jax.random.uniform(seeds[15], (D,), jnp.float32) ** shard_levels(seeds[15], (D,), ((0, 16),), -0.2, 0.2)), 0.5, 2.0),
    }


EPSILON = 1e-06

def normalize_rows(token_rows, gain_vector):
    values = token_rows.astype(jnp.float32)
    scaled = values * lax.rsqrt(lax.optimization_barrier(jnp.mean(values * values, axis=-1, keepdims=True)) + EPSILON)
    return (scaled * gain_vector).astype(jnp.bfloat16)

def split_sum(left, right, column_scale, shard_count):
    shard_width = left.shape[1] // shard_count
    running = jnp.zeros((left.shape[0], right.shape[1]), jnp.float32)
    for shard_index in range(shard_count):
        low = shard_index * shard_width
        partial_value = jnp.dot(left[:, low:low + shard_width], right[low:low + shard_width, :], preferred_element_type=jnp.float32) * column_scale
        rounded = lax.optimization_barrier(partial_value.astype(jnp.bfloat16))
        running = running + rounded.astype(jnp.float32)
    return running

def reference(tokens, mixer_gain, w_content, w_spatial, content_scale, spatial_scale, spatial_gain, block_mixing, block_bias, w_project, project_scale, channel_gain, w_up, up_scale, w_down, down_scale):
    content_weight = w_content.astype(jnp.bfloat16)
    spatial_weight = w_spatial.astype(jnp.bfloat16)
    project_weight = w_project.astype(jnp.bfloat16)
    up_weight = w_up.astype(jnp.bfloat16)
    down_weight = w_down.astype(jnp.bfloat16)
    causal_mask = jnp.tril(jnp.ones((BLOCK, BLOCK), dtype=bool))
    mixing_weights = jnp.where(causal_mask[None, :, :], block_mixing.astype(jnp.float32), jnp.float32(0.0))

    def one_sequence(token_rows):
        normed = normalize_rows(token_rows, mixer_gain)
        content = jax.nn.gelu(jnp.dot(normed, content_weight, preferred_element_type=jnp.float32) * content_scale)
        spatial = jax.nn.gelu(jnp.dot(normed, spatial_weight, preferred_element_type=jnp.float32) * spatial_scale)
        spatial_norm = (spatial * lax.rsqrt(lax.optimization_barrier(jnp.mean(spatial * spatial, axis=-1, keepdims=True)) + EPSILON) * spatial_gain).astype(jnp.bfloat16)
        grouped = spatial_norm.astype(jnp.float32).reshape(TOK_DEV // BLOCK, BLOCK, GROUPS, GCH)
        mixed_block = jnp.einsum('gts,nsgc->ntgc', mixing_weights, grouped) + block_bias.T[None, :, :, None]
        gated = (content * mixed_block.reshape(TOK_DEV, W_SGU)).astype(jnp.bfloat16)
        mixer_sum = split_sum(gated, project_weight, project_scale, N_TP)
        middle = (token_rows.astype(jnp.float32) + mixer_sum).astype(jnp.bfloat16)
        channel_normed = normalize_rows(middle, channel_gain)
        up_linear = jnp.dot(channel_normed, up_weight, preferred_element_type=jnp.float32) * up_scale
        hidden = jnp.square(jax.nn.relu(up_linear)).astype(jnp.bfloat16)
        channel_sum = split_sum(hidden, down_weight, down_scale, N_TP)
        return (middle.astype(jnp.float32) + channel_sum).astype(jnp.bfloat16)
    layer_out = lax.map(one_sequence, tokens.reshape(N_FS, TOK_DEV, D))
    return layer_out.reshape(TOKENS, D)
```

```python
import jax
import jax.numpy as jnp
from jax import lax
from jax.sharding import PartitionSpec as P

EPSILON = 1e-06
BF16 = jnp.bfloat16
F32 = jnp.float32


def normalize_rows(token_rows, gain_vector):
    values = token_rows.astype(F32)
    scaled = values * lax.rsqrt(jnp.mean(values * values, axis=-1, keepdims=True) + EPSILON)
    return (scaled * gain_vector).astype(BF16)


def plane_size(fs_size):
    size = 1
    while size < 4 and fs_size % (2 * size) == 0:
        size *= 2
    return size


def shards(
    tokens,
    mixer_gain,
    w_content,
    w_spatial,
    content_scale,
    spatial_scale,
    spatial_gain,
    block_mixing,
    block_bias,
    w_project,
    project_scale,
    channel_gain,
    w_up,
    up_scale,
    w_down,
    down_scale,
):
    fs_size, tp_size = lax.axis_size("fs"), lax.axis_size("tp")
    plane = plane_size(fs_size)
    depth = fs_size // plane
    bits = [1 << i for i in range(plane.bit_length() - 1)]
    fs_index, tp_index = lax.axis_index("fs"), lax.axis_index("tp")
    a_index, b_index = fs_index % plane, fs_index // plane

    def partner(value, flip):
        return lax.ppermute(value, "fs", [(i, i ^ flip) for i in range(fs_size)])

    def deeper(value):
        return lax.ppermute(value, "fs", [(i, (i + plane) % fs_size) for i in range(fs_size)])

    def tp_other(value):
        return lax.ppermute(value, "tp", [(0, 1), (1, 0)])

    def tp_gather_columns(value):
        if tp_size != 2:
            return lax.all_gather(value, "tp", axis=1, tiled=True)
        other = tp_other(value)
        first = tp_index == 0
        return jnp.concatenate(
            [jnp.where(first, value, other), jnp.where(first, other, value)], axis=1
        )

    def tp_scatter_columns(value):
        if tp_size != 2:
            return lax.psum_scatter(
                value.astype(BF16), "tp", scatter_dimension=1, tiled=True
            ).astype(F32)
        half = value.shape[1] // 2
        low, high = value[:, :half].astype(BF16), value[:, half:].astype(BF16)
        first = tp_index == 0
        received = tp_other(jnp.where(first, high, low))
        return jnp.where(first, low, high).astype(F32) + received.astype(F32)

    def gather_plane(value, order):
        dims = value.shape
        held = value.reshape((1,) * len(bits) + dims)
        for bit in order:
            axis = len(bits) - bit.bit_length()
            other = partner(held, bit)
            first = (a_index & bit) == 0
            held = jnp.concatenate(
                [jnp.where(first, held, other), jnp.where(first, other, held)], axis=axis
            )
        return held.reshape((plane,) + dims)

    def exchange_plane(pieces):
        received = [lax.dynamic_index_in_dim(pieces, a_index, 0, keepdims=False)]
        for flip in range(1, plane):
            received.append(
                partner(lax.dynamic_index_in_dim(pieces, a_index ^ flip, 0, keepdims=False), flip)
            )
        for bit in bits:
            swap = (a_index & bit) != 0
            received = [jnp.where(swap, received[k ^ bit], received[k]) for k in range(plane)]
        return received

    def place(full, block, step, axis):
        where = ((b_index - step) % depth) * block.shape[axis]
        return lax.dynamic_update_slice_in_dim(full, block, where, axis)

    content_weight = w_content.astype(BF16)
    spatial_weight = w_spatial.astype(BF16)
    project_weight = (w_project.astype(BF16).astype(F32) * project_scale).astype(BF16).T
    width = content_weight.shape[1]
    half = width // 2
    first_color = jnp.concatenate([content_weight, project_weight[:, :half]], axis=1)
    second_color = jnp.concatenate([spatial_weight, project_weight[:, half:]], axis=1)
    rows_here = content_weight.shape[0]
    model_width = rows_here * fs_size
    content_full = jnp.zeros((model_width, width), BF16)
    spatial_full = jnp.zeros((model_width, width), BF16)
    project_full = jnp.zeros((model_width, width), BF16)
    for step in range(depth):
        first_rows = gather_plane(first_color, bits).reshape(plane * rows_here, -1)
        second_rows = gather_plane(second_color, bits[::-1]).reshape(plane * rows_here, -1)
        content_full = place(content_full, first_rows[:, :width], step, 0)
        spatial_full = place(spatial_full, second_rows[:, :width], step, 0)
        project_full = place(
            project_full,
            jnp.concatenate([first_rows[:, width:], second_rows[:, width:]], axis=1),
            step,
            0,
        )
        if step < depth - 1:
            first_color, second_color = deeper(first_color), deeper(second_color)

    hidden_here = w_up.shape[1] // plane
    up_pieces = w_up.astype(BF16).reshape(rows_here, plane, hidden_here).transpose(1, 0, 2)
    up_block = jnp.concatenate(exchange_plane(up_pieces), axis=0)
    down_scaled = (w_down.astype(BF16).astype(F32) * down_scale).astype(BF16)
    down_pieces = down_scaled.reshape(plane, hidden_here, rows_here)
    down_block = jnp.concatenate(exchange_plane(down_pieces), axis=1)
    up_block, down_block, _, _ = lax.optimization_barrier(
        (up_block, down_block, first_color, second_color)
    )
    up_full = jnp.zeros((model_width, hidden_here), BF16)
    down_full = jnp.zeros((hidden_here, model_width), BF16)
    for step in range(depth):
        up_full = place(up_full, up_block, step, 0)
        if step < depth - 1:
            up_block = deeper(up_block)
    down_block, _ = lax.optimization_barrier((down_block, up_block))
    for step in range(depth):
        down_full = place(down_full, down_block, step, 1)
        if step < depth - 1:
            down_block = deeper(down_block)

    normed = normalize_rows(tp_gather_columns(tokens), mixer_gain)
    row_count = normed.shape[0]
    content = jax.nn.gelu(
        jnp.dot(normed, content_full, preferred_element_type=F32) * content_scale
    )
    spatial = jax.nn.gelu(
        jnp.dot(normed, spatial_full, preferred_element_type=F32) * spatial_scale
    )
    square_sums = jnp.sum(spatial * spatial, axis=1)
    if tp_size == 2:
        square_sums = square_sums + tp_other(square_sums)
    else:
        square_sums = lax.psum(square_sums, "tp")
    spatial_norm = (
        spatial * lax.rsqrt(square_sums / (width * tp_size) + EPSILON)[:, None] * spatial_gain
    ).astype(BF16)
    groups_here, block_size = block_mixing.shape[0], block_mixing.shape[1]
    group_width = width // groups_here
    causal_mask = jnp.tril(jnp.ones((block_size, block_size), dtype=bool))
    mixing_weights = jnp.where(causal_mask[None, :, :], block_mixing, jnp.zeros_like(block_mixing))
    grouped = spatial_norm.reshape(row_count // block_size, block_size, groups_here, group_width)
    mixed_block = (
        jnp.einsum("gts,nsgc->ntgc", mixing_weights, grouped, preferred_element_type=F32)
        + block_bias.T[None, :, :, None]
    )
    gated = (content * mixed_block.reshape(row_count, width)).astype(BF16)
    mixer_terms = lax.dot_general(
        gated, project_full, (((1,), (1,)), ((), ())), preferred_element_type=F32
    )
    middle = (tokens.astype(F32) + tp_scatter_columns(mixer_terms)).astype(BF16)

    middle_rows = tp_gather_columns(middle)
    own_rows = normalize_rows(middle_rows, channel_gain)
    columns_here = middle.shape[1]
    own_columns = lax.dynamic_slice_in_dim(own_rows, tp_index * columns_here, columns_here, 1)
    up_scale_here = lax.dynamic_slice_in_dim(up_scale, a_index * hidden_here, hidden_here, 0)
    arrived = [partner(own_columns, flip) for flip in range(1, plane)]
    total = middle.astype(F32)
    for flip in range(plane):
        rows = own_rows if flip == 0 else tp_gather_columns(arrived[flip - 1])
        up_linear = jnp.dot(rows, up_full, preferred_element_type=F32)
        hidden = jnp.square(jax.nn.relu(up_linear * up_scale_here)).astype(BF16)
        terms = tp_scatter_columns(jnp.dot(hidden, down_full, preferred_element_type=F32))
        if flip > 0:
            terms = partner(terms.astype(BF16), flip).astype(F32)
        total = total + terms
    return total.astype(BF16)


def solution(mesh):
    return jax.shard_map(
        shards,
        mesh=mesh,
        in_specs=(
            P("fs", "tp"),
            P(),
            P("fs", "tp"),
            P("fs", "tp"),
            P("tp"),
            P("tp"),
            P("tp"),
            P("tp", None, None),
            P("tp", None),
            P("tp", "fs"),
            P("fs"),
            P(),
            P("fs", "tp"),
            P("tp"),
            P("tp", "fs"),
            P("fs"),
        ),
        out_specs=P("fs", "tp"),
        check_vma=False,
    )
```

```python
import jax
import jax.numpy as jnp
from jax import lax
from jax.sharding import PartitionSpec as P

EPSILON = 1e-06
BF16 = jnp.bfloat16
F32 = jnp.float32


def normalize_rows(token_rows, gain_vector):
    values = token_rows.astype(F32)
    scaled = values * lax.rsqrt(jnp.mean(values * values, axis=-1, keepdims=True) + EPSILON)
    return (scaled * gain_vector).astype(BF16)


def plane_size(fs_size):
    size = 1
    while size < 4 and fs_size % (2 * size) == 0:
        size *= 2
    return size


def shards(
    tokens,
    mixer_gain,
    w_content,
    w_spatial,
    content_scale,
    spatial_scale,
    spatial_gain,
    block_mixing,
    block_bias,
    w_project,
    project_scale,
    channel_gain,
    w_up,
    up_scale,
    w_down,
    down_scale,
):
    fs_size, tp_size = lax.axis_size("fs"), lax.axis_size("tp")
    plane = plane_size(fs_size)
    depth = fs_size // plane
    bits = [1 << i for i in range(plane.bit_length() - 1)]
    fs_index, tp_index = lax.axis_index("fs"), lax.axis_index("tp")
    a_index, b_index = fs_index % plane, fs_index // plane

    def partner(value, flip):
        return lax.ppermute(value, "fs", [(i, i ^ flip) for i in range(fs_size)])

    def deeper(value):
        return lax.ppermute(value, "fs", [(i, (i + plane) % fs_size) for i in range(fs_size)])

    def tp_other(value):
        return lax.ppermute(value, "tp", [(0, 1), (1, 0)])

    def tp_gather_columns(value):
        if tp_size != 2:
            return lax.all_gather(value, "tp", axis=1, tiled=True)
        other = tp_other(value)
        first = tp_index == 0
        return jnp.concatenate(
            [jnp.where(first, value, other), jnp.where(first, other, value)], axis=1
        )

    def tp_scatter_columns(value):
        if tp_size != 2:
            return lax.psum_scatter(
                value.astype(BF16), "tp", scatter_dimension=1, tiled=True
            ).astype(F32)
        half = value.shape[1] // 2
        low, high = value[:, :half].astype(BF16), value[:, half:].astype(BF16)
        first = tp_index == 0
        received = tp_other(jnp.where(first, high, low))
        return jnp.where(first, low, high).astype(F32) + received.astype(F32)

    def gather_plane(value, order):
        dims = value.shape
        held = value.reshape((1,) * len(bits) + dims)
        for bit in order:
            axis = len(bits) - bit.bit_length()
            other = partner(held, bit)
            first = (a_index & bit) == 0
            held = jnp.concatenate(
                [jnp.where(first, held, other), jnp.where(first, other, held)], axis=axis
            )
        return held.reshape((plane,) + dims)

    def exchange_plane(value, axis):
        size = value.shape[axis] // plane

        def piece(index):
            return lax.dynamic_slice_in_dim(value, index * size, size, axis)

        received = [piece(a_index)]
        for flip in range(1, plane):
            received.append(partner(piece(a_index ^ flip), flip))
        for bit in bits:
            swap = (a_index & bit) != 0
            received = [jnp.where(swap, received[k ^ bit], received[k]) for k in range(plane)]
        return received

    def place(full, block, step, axis):
        where = ((b_index - step) % depth) * block.shape[axis]
        return lax.dynamic_update_slice_in_dim(full, block, where, axis)

    content_weight = w_content.astype(BF16)
    spatial_weight = w_spatial.astype(BF16)
    project_weight = (w_project.astype(BF16).astype(F32) * project_scale).astype(BF16).T
    width = content_weight.shape[1]
    half = width // 2
    rows_here = content_weight.shape[0]
    model_width = rows_here * fs_size
    wire = width + half
    held = [
        jnp.concatenate(
            [content_weight, project_weight[:, :half], spatial_weight, project_weight[:, half:]],
            axis=1,
        )
    ]
    for _ in range(1, depth):
        held.append(deeper(held[-1]))

    hidden_here = w_up.shape[1] // plane
    up_block = jnp.concatenate(exchange_plane(w_up.astype(BF16), 1), axis=0)
    up_block, _ = lax.optimization_barrier((up_block, held[-2] if depth > 2 else held[-1]))
    up_full = jnp.zeros((model_width, hidden_here), BF16)
    for step in range(depth):
        up_full = place(up_full, up_block, step, 0)
        if step < depth - 1:
            up_block = deeper(up_block)

    content_full = jnp.zeros((model_width, width), BF16)
    spatial_full = jnp.zeros((model_width, width), BF16)
    project_full = jnp.zeros((model_width, width), BF16)
    for low in range(0, depth, 2):
        both = jnp.stack(held[low : low + 2])
        first_rows = gather_plane(both[:, :, :wire], bits)
        second_rows = gather_plane(both[:, :, wire:], bits[::-1])
        for at in range(both.shape[0]):
            first = first_rows[:, at].reshape(plane * rows_here, wire)
            second = second_rows[:, at].reshape(plane * rows_here, wire)
            content_full = place(content_full, first[:, :width], low + at, 0)
            spatial_full = place(spatial_full, second[:, :width], low + at, 0)
            project_full = place(
                project_full,
                jnp.concatenate([first[:, width:], second[:, width:]], axis=1),
                low + at,
                0,
            )

    down_scaled = (w_down.astype(BF16).astype(F32) * down_scale).astype(BF16)
    down_scaled, _, _ = lax.optimization_barrier((down_scaled, first_rows, second_rows))
    down_block = jnp.concatenate(exchange_plane(down_scaled, 0), axis=1)
    down_blocks = [down_block]
    for _ in range(1, depth):
        down_blocks.append(deeper(down_blocks[-1]))

    normed = normalize_rows(tp_gather_columns(tokens), mixer_gain)
    row_count = normed.shape[0]
    content = jax.nn.gelu(
        jnp.dot(normed, content_full, preferred_element_type=F32) * content_scale
    )
    spatial = jax.nn.gelu(
        jnp.dot(normed, spatial_full, preferred_element_type=F32) * spatial_scale
    )
    square_sums = jnp.sum(spatial * spatial, axis=1)
    if tp_size == 2:
        square_sums = square_sums + tp_other(square_sums)
    else:
        square_sums = lax.psum(square_sums, "tp")
    spatial_norm = (
        spatial * lax.rsqrt(square_sums / (width * tp_size) + EPSILON)[:, None] * spatial_gain
    ).astype(BF16)
    groups_here, block_size = block_mixing.shape[0], block_mixing.shape[1]
    group_width = width // groups_here
    causal_mask = jnp.tril(jnp.ones((block_size, block_size), dtype=bool))
    mixing_weights = jnp.where(causal_mask[None, :, :], block_mixing, jnp.zeros_like(block_mixing))
    grouped = spatial_norm.reshape(row_count // block_size, block_size, groups_here, group_width)
    mixed_block = (
        jnp.einsum("gts,nsgc->ntgc", mixing_weights, grouped, preferred_element_type=F32)
        + block_bias.T[None, :, :, None]
    )
    gated = (content * mixed_block.reshape(row_count, width)).astype(BF16)
    mixer_terms = lax.dot_general(
        gated, project_full, (((1,), (1,)), ((), ())), preferred_element_type=F32
    )
    middle = (tokens.astype(F32) + tp_scatter_columns(mixer_terms)).astype(BF16)

    middle_rows = tp_gather_columns(middle)
    own_rows = normalize_rows(middle_rows, channel_gain)
    columns_here = middle.shape[1]
    own_columns = lax.dynamic_slice_in_dim(own_rows, tp_index * columns_here, columns_here, 1)
    up_scale_here = lax.dynamic_slice_in_dim(up_scale, a_index * hidden_here, hidden_here, 0)
    arrived = []
    for flip in range(1, plane):
        arrived.append(partner(own_columns, flip))
    hidden_rows = []
    for flip in range(plane):
        rows = own_rows if flip == 0 else tp_gather_columns(arrived[flip - 1])
        up_linear = jnp.dot(rows, up_full, preferred_element_type=F32)
        hidden_rows.append(jnp.square(jax.nn.relu(up_linear * up_scale_here)).astype(BF16))
    hidden = jnp.concatenate(hidden_rows, axis=0)

    def plane_sum(terms):
        total = terms[:row_count]
        for flip in range(1, plane):
            sent = terms[flip * row_count : (flip + 1) * row_count].astype(BF16)
            total = total + partner(sent, flip).astype(F32)
        return total

    if tp_size != 2 or depth % 2:
        down_full = jnp.zeros((hidden_here, model_width), BF16)
        for step in range(depth):
            down_full = place(down_full, down_blocks[step], step, 1)
        terms = tp_scatter_columns(jnp.dot(hidden, down_full, preferred_element_type=F32))
        return (middle.astype(F32) + plane_sum(terms)).astype(BF16)

    sums = []
    for step in range(depth):
        terms = jnp.dot(hidden, down_blocks[step], preferred_element_type=F32)
        terms = tp_scatter_columns(terms)
        sums.append(plane_sum(terms))
    ordered = [sums[-k % depth] for k in range(depth)]
    bit = 1
    while bit < depth:
        turn = (b_index & bit) != 0
        ordered = [jnp.where(turn, ordered[(k - bit) % depth], ordered[k]) for k in range(depth)]
        bit *= 2
    half_depth = depth // 2
    low = jnp.stack(ordered[:half_depth])
    high = jnp.stack(ordered[half_depth:])
    first = tp_index == 0
    received = tp_other(jnp.where(first, high, low))
    mine = jnp.where(first, low, high)
    left, right = jnp.where(first, mine, received), jnp.where(first, received, mine)
    pieces = [side[k] for k in range(half_depth) for side in (left, right)]
    return (middle.astype(F32) + jnp.concatenate(pieces, axis=1)).astype(BF16)


def solution(mesh):
    return jax.shard_map(
        shards,
        mesh=mesh,
        in_specs=(
            P("fs", "tp"),
            P(),
            P("fs", "tp"),
            P("fs", "tp"),
            P("tp"),
            P("tp"),
            P("tp"),
            P("tp", None, None),
            P("tp", None),
            P("tp", "fs"),
            P("fs"),
            P(),
            P("fs", "tp"),
            P("tp"),
            P("tp", "fs"),
            P("fs"),
        ),
        out_specs=P("fs", "tp"),
        check_vma=False,
    )
```
